32 devices in a mesh: kv: 8 (over z, x), tp: 4 (over y, core).
Axes of the slice: x: 2, y: 2, z: 4, core: 2. Of those that a mesh axis runs over, the one named last changes fastest.
Arguments:
- tokens: bfloat16 [1024, 2048], P('kv', 'tp'), may hold values from -6 to 6
- states: float32 [1024, 16, 64, 64], P('kv', 'tp'), may hold values from -6 to 6
- mix_gain: bfloat16 [2048], replicated, may hold values from 0.099609375 to 1.8984375
- w_query: bfloat16 [2048, 1024], P(None, 'tp'), may hold values from -0.125 to 0.125
- w_key: bfloat16 [2048, 1024], P(None, 'tp'), may hold values from -0.125 to 0.125
- w_value: bfloat16 [2048, 1024], P(None, 'tp'), may hold values from -0.125 to 0.125
- w_gate: bfloat16 [2048, 1024], P(None, 'tp'), may hold values from -0.125 to 0.125
- head_gain: bfloat16 [1024], P('tp'), may hold values from 0.099609375 to 1.8984375
- w_output: bfloat16 [1024, 2048], P('tp'), may hold values from -0.1875 to 0.1875
- channel_gain: bfloat16 [2048], replicated, may hold values from 0.099609375 to 1.8984375
- w_up: bfloat16 [2048, 8192], P(None, 'kv'), may hold values from -0.125 to 0.125
- w_down: bfloat16 [8192, 2048], P('kv'), may hold values from -0.0625 to 0.0625
Outputs:
- layer_out: bfloat16 [1024, 2048], P('kv', 'tp')
- new_states: float32 [1024, 16, 64, 64], P('kv', 'tp')
The draws below stay inside these ranges and needn't reach their ends.
All inputs are finite; a program needn't handle non-finite values.
Results may differ from the reference program's by a relative error of at most 0.019.
Values may be sent and summed in bfloat16 or wider, within the bound.
A program may use at most 64 MiB of HBM per device.

```python
import jax
import jax.numpy as jnp
from jax import lax

D = 2048
HEADS = 16
HEAD = 64
FF = 8192
POS = 16384
BATCH = 1024
N_TP = 4


def draw_tokens(key, part):
    first_key = jax.random.fold_in(jax.random.fold_in(key, 11), 0)
    column = jnp.arange(D, dtype=jnp.float32) / D
    profile = 0.5 * jnp.exp(jnp.log(3.0) * column)
    drawn = jax.random.normal(first_key, (BATCH, D), jnp.float32) * profile
    return jnp.clip(drawn, -6.0, 6.0).astype(jnp.bfloat16)


def shard_levels(rng, extent, shards, smallest, high):
    gain = 1.0
    for dim, parts in shards:
        steps = jax.random.uniform(jax.random.fold_in(jax.random.fold_in(rng, 6), dim), (parts,), jnp.float32, smallest / len(shards), high / len(shards))
        gain = gain * jnp.repeat(jnp.exp(steps), extent[dim] // parts).reshape((-1,) + (1,) * (len(extent) - 1 - dim))
    return gain


def scatter_about(rng, extent, scale, bound, shards=(), kind=jnp.bfloat16):
    array = jax.random.normal(rng, extent, jnp.float32) * scale
    if len(shards) > 0:
        array = shard_levels(rng, extent, shards, -0.22, 0.18) * array
    return jnp.clip(array, min=-bound, max=bound).astype(kind)


def setup_inputs(seed: int = 0) -> dict:
    arg_keys = jax.random.split(jax.random.key(seed), 13)
    return {
        "tokens": draw_tokens(jax.random.fold_in(arg_keys[12], 71), 0),
        "states": scatter_about(arg_keys[1], (BATCH, HEADS, HEAD, HEAD), 1.0, 6.0, ((0, 8), (1, 4)), jnp.float32),
        "mix_gain": jnp.clip(1.0 + 0.18 * jax.random.normal(arg_keys[2], (D,), jnp.float32), 0.099609375, 1.8984375).astype(jnp.bfloat16),
        "w_query": scatter_about(arg_keys[3], (D, HEADS * HEAD), D ** -0.5, 0.125, ((1, 4),)),
        "w_key": scatter_about(arg_keys[4], (D, HEADS * HEAD), D ** -0.5, 0.125, ((1, 4),)),
        "w_value": scatter_about(arg_keys[5], (D, HEADS * HEAD), D ** -0.5, 0.125, ((1, 4),)),
        "w_gate": scatter_about(arg_keys[6], (D, HEADS * HEAD), D ** -0.5, 0.125, ((1, 4),)),
        "head_gain": jnp.clip(1.0 + 0.18 * jax.random.normal(arg_keys[7], (HEADS * HEAD,), jnp.float32), 0.099609375, 1.8984375).astype(jnp.bfloat16),
        "w_output": scatter_about(arg_keys[8], (HEADS * HEAD, D), (HEADS * HEAD) ** -0.5, 0.1875, ((0, 4),)),
        "channel_gain": jnp.clip(1.0 + 0.18 * jax.random.normal(arg_keys[9], (D,), jnp.float32), 0.099609375, 1.8984375).astype(jnp.bfloat16),
        "w_up": scatter_about(arg_keys[10], (D, FF), D ** -0.5, 0.125, ((1, 8),)),
        "w_down": scatter_about(arg_keys[11], (FF, D), FF ** -0.5, 0.0625, ((0, 8),)),
    }


EPSILON = 1e-06
ROTARY_BASE = 10000.0

def rotate(vectors):
    half_size = vectors.shape[-1] // 2
    frequency = ROTARY_BASE ** (-jnp.arange(half_size, dtype=jnp.float32) / half_size)
    angles = POS * frequency
    cosine = jnp.cos(angles)
    sines = jnp.sin(angles)
    first_half = vectors[..., :half_size]
    second = vectors[..., half_size:]
    return jnp.concatenate([first_half * cosine - second * sines, first_half * sines + second * cosine], axis=-1)

def retain(normed, states, w_query, w_key, w_value, w_gate, head_gain, head_ids):
    row_count = states.shape[0]
    head_count = states.shape[1]
    head_size = states.shape[2]

    def project(weight):
        return jnp.dot(normed, weight, preferred_element_type=jnp.float32).reshape(row_count, head_count, head_size)
    queries = rotate(project(w_query)) * head_size ** (-0.5)
    keys_now = rotate(project(w_key))
    values = project(w_value)
    gating = jnp.dot(normed, w_gate, preferred_element_type=jnp.float32)
    decays = 1.0 - jnp.exp2(-1.0 - 11.0 * head_ids / (HEADS - 1))
    new_states = decays[None, :, None, None] * states + keys_now[:, :, :, None] * values[:, :, None, :]
    output = jnp.einsum('bhk,bhkv->bhv', queries, new_states, precision=lax.Precision.HIGHEST)
    center = output - lax.optimization_barrier(jnp.mean(output, axis=-1, keepdims=True))
    spread = lax.optimization_barrier(jnp.mean(center * center, axis=-1, keepdims=True))
    scaled = center * lax.rsqrt(spread + EPSILON) * head_gain.astype(jnp.float32).reshape(head_count, head_size)
    gated_out = (scaled.reshape(row_count, head_count * head_size) * jax.nn.silu(gating)).astype(jnp.bfloat16)
    return (gated_out, new_states)

def reference(tokens, states, mix_gain, w_query, w_key, w_value, w_gate, head_gain, w_output, channel_gain, w_up, w_down):
    widened = tokens.astype(jnp.float32)
    inverse_rms = lax.rsqrt(lax.optimization_barrier(jnp.mean(widened * widened, axis=1, keepdims=True)) + EPSILON)
    normed = (widened * inverse_rms * mix_gain.astype(jnp.float32)).astype(jnp.bfloat16)
    head_ids = jnp.arange(HEADS).astype(jnp.float32)
    gated_out, new_states = retain(normed, states, w_query, w_key, w_value, w_gate, head_gain, head_ids)
    blocks = gated_out.astype(jnp.float32).reshape(BATCH, N_TP, -1)
    weights = w_output.astype(jnp.float32).reshape(N_TP, -1, D)
    partials = jnp.einsum('btc,tcd->btd', blocks, weights)
    rounded = lax.optimization_barrier(partials.astype(jnp.bfloat16))
    attended = lax.optimization_barrier(jnp.sum(rounded.astype(jnp.float32), axis=1))
    middle = (widened + attended).astype(jnp.bfloat16)
    mid_wide = middle.astype(jnp.float32)
    second_rms = lax.rsqrt(lax.optimization_barrier(jnp.mean(mid_wide * mid_wide, axis=1, keepdims=True)) + EPSILON)
    scaled = (mid_wide * channel_gain.astype(jnp.float32)).astype(jnp.bfloat16)
    hidden = jnp.dot(scaled, w_up, preferred_element_type=jnp.float32) * second_rms
    activated = jnp.square(jax.nn.relu(hidden)).astype(jnp.bfloat16)
    down_sum = jnp.dot(activated, w_down, preferred_element_type=jnp.float32)
    layer_out = (mid_wide + down_sum).astype(jnp.bfloat16)
    return (layer_out, new_states)
```

```python
import functools
import math

import jax
import jax.numpy as jnp
import numpy as np
from jax import lax
from jax.experimental import pallas as pl
from jax.experimental.pallas import tpu as pltpu
from jax.sharding import PartitionSpec as P

POS = 16384
EPSILON = 1e-06
ROTARY_BASE = 10000.0
CORES = 2
CHUNKS = 2
MESH = pl.DeviceIdType.MESH
F32 = jnp.float32
BF16 = jnp.bfloat16


def dot(a, b):
    return jnp.dot(a, b, preferred_element_type=F32)


def kernel(
    sizes,
    tok_hbm, st_hbm, mix_gain, wq_hbm, wk_hbm, wv_hbm, wg_hbm, head_gain, wo_hbm,
    chan_gain, wu_hbm, wd_hbm, turn,
    out_ref, new_hbm,
    xf, wproj, st, wo, wu, wd, acc, qt, kt, vt, rt,
    part, r1, s2, r2, mid, lhs, act, sx, rx, sz, rz, fin, ob,
    load_sem, store_sem, a_send, a_recv, b1_send, b1_recv, b2_send, b2_recv,
    cz_send, cx_send, c_recv, dx_send, dx_recv, dz_send, dz_recv, e_send, e_recv,
):
    n_tp, ny, nz, nx, heads, head, rows, feats, share, width = sizes
    tp = lax.axis_index("tp")
    kv = lax.axis_index("kv")
    c, y = lax.rem(tp, CORES), tp // CORES
    x, z = lax.rem(kv, nx), kv // nx
    other = 1 - c
    partner = y * CORES + other
    half = head // 2
    piece = width // CHUNKS
    sent = []

    def ys(d):
        return lax.rem(y + d, ny)

    def zs(d):
        return lax.rem(z + d, nz)

    def xs(d):
        return lax.rem(x + d, nx)

    def make(src, dst, ssem, rsem, device):
        return pltpu.make_async_remote_copy(
            src_ref=src, dst_ref=dst, send_sem=ssem, recv_sem=rsem,
            device_id=device, device_id_type=MESH,
        )

    def send(src, dst, ssem, rsem, device):
        copy = make(src, dst, ssem, rsem, device)
        copy.start()
        sent.append(copy)

    def arrive(dst, ssem, rsem, device):
        make(dst, dst, ssem, rsem, device).wait_recv()

    barrier = pltpu.get_barrier_semaphore()
    greeted = 0
    for d in range(1, n_tp):
        pl.semaphore_signal(barrier, inc=1, device_id={"tp": lax.rem(tp + d, n_tp)}, device_id_type=MESH)
        greeted += 1
    for d in range(1, nx):
        pl.semaphore_signal(barrier, inc=1, device_id={"kv": z * nx + xs(d)}, device_id_type=MESH)
        greeted += 1
    for d in range(1, nz):
        pl.semaphore_signal(barrier, inc=1, device_id={"kv": zs(d) * nx + x}, device_id_type=MESH)
        greeted += 1

    loads = [pltpu.make_async_copy(tok_hbm, xf.at[tp], load_sem.at[0])]
    for i, w in enumerate((wq_hbm, wk_hbm, wv_hbm, wg_hbm)):
        loads.append(pltpu.make_async_copy(w, wproj.at[i], load_sem.at[1 + i]))
    for h in range(heads):
        loads.append(pltpu.make_async_copy(st_hbm.at[h], st.at[h], load_sem.at[5 + h]))
    loads.append(pltpu.make_async_copy(wo_hbm, wo, load_sem.at[5 + heads]))
    loads.append(pltpu.make_async_copy(wu_hbm, wu, load_sem.at[6 + heads]))
    loads.append(pltpu.make_async_copy(wd_hbm, wd, load_sem.at[7 + heads]))
    for copy in loads:
        copy.start()
    loads[0].wait()
    pl.semaphore_wait(barrier, greeted)

    for d in range(1, ny):
        send(xf.at[tp], xf.at[tp], a_send.at[d], a_recv.at[tp], {"tp": ys(d) * CORES + c})
    send(xf.at[tp], xf.at[tp], a_send.at[0], a_recv.at[tp], {"tp": partner})

    squares = jnp.zeros((rows, 1), F32)

    def project(slot, first, squares):
        at = pl.ds(pl.multiple_of(slot * feats, feats), feats)
        wide = xf[slot].astype(F32)
        scaled = (wide * mix_gain[:, at].astype(F32)).astype(BF16)
        for i in range(4):
            if first:
                loads[1 + i].wait()
            term = dot(scaled, wproj[i, at, :])
            if first:
                acc[i] = term
            else:
                acc[i] += term
        return squares + jnp.sum(wide * wide, axis=1, keepdims=True)

    squares = project(tp, True, squares)
    arrive(xf.at[partner], a_send.at[0], a_recv.at[partner], {"tp": partner})
    squares = project(partner, False, squares)
    for d in range(1, ny):
        slot = ys(d) * CORES + c
        arrive(xf.at[slot], a_send.at[0], a_recv.at[slot], {"tp": slot})
        send(xf.at[slot], xf.at[slot], a_send.at[ny + d], a_recv.at[slot], {"tp": partner})
        squares = project(slot, False, squares)
        slot = ys(d) * CORES + other
        arrive(xf.at[slot], a_send.at[0], a_recv.at[slot], {"tp": partner})
        squares = project(slot, False, squares)
    inverse = lax.rsqrt(squares * (1.0 / width) + EPSILON)

    qt[...] = (acc[0] * inverse).T
    kt[...] = (acc[1] * inverse).T
    vt[...] = (acc[2] * inverse).T
    cosine, sine = turn[:half, :], turn[half:, :]
    for h in range(heads):
        lo, hi = pl.ds(h * head, half), pl.ds(h * head + half, half)
        for ref, scale in ((qt, head ** -0.5), (kt, 1.0)):
            a, b = ref[lo, :], ref[hi, :]
            ref[lo, :] = (a * cosine - b * sine) * scale
            ref[hi, :] = (a * sine + b * cosine) * scale
    stores = []
    for h in range(heads):
        loads[5 + h].wait()
        number = (tp * heads + h).astype(F32)
        decay = 1.0 - jnp.exp2(-1.0 - 11.0 * jnp.full((1, rows), number, F32) / (heads * n_tp - 1))
        value = vt[pl.ds(h * head, head), :]
        base = h * head

        def step(k, total, h=h, base=base, decay=decay, value=value):
            fresh = decay * st[h, k] + kt[pl.ds(base + k, 1), :] * value
            st[h, k] = fresh
            return total + qt[pl.ds(base + k, 1), :] * fresh

        total = lax.fori_loop(0, head, step, jnp.zeros((head, rows), F32), unroll=8)
        center = total - jnp.mean(total, axis=0, keepdims=True)
        spread = jnp.mean(center * center, axis=0, keepdims=True)
        rt[pl.ds(base, head), :] = center * lax.rsqrt(spread + EPSILON)
        copy = pltpu.make_async_copy(st.at[h], new_hbm.at[h], store_sem.at[h])
        copy.start()
        stores.append(copy)
    gating = acc[3] * inverse
    gated = (rt[...].T * head_gain[...].astype(F32) * (gating * jax.nn.sigmoid(gating))).astype(BF16)

    loads[5 + heads].wait()
    for j in range(CHUNKS):
        whole = dot(gated, wo[:, j * piece:(j + 1) * piece]).astype(BF16)
        for t in range(n_tp):
            part[j, t] = whole[t * share:(t + 1) * share]
        for d in range(ny):
            to = ys(d)
            send(part.at[j, to * CORES + other], r1.at[j, to], b1_send.at[j, d], b1_recv.at[j, to], {"tp": partner})

    def pair_sum(j, to):
        arrive(r1.at[j, to], b1_send.at[0, 0], b1_recv.at[j, to], {"tp": partner})
        return part[j, to * CORES + c].astype(F32) + r1[j, to].astype(F32)

    for j in range(CHUNKS):
        for d in range(1, ny):
            to = ys(d)
            s2[j, to] = pair_sum(j, to).astype(BF16)
            send(s2.at[j, to], r2.at[j, y], b2_send.at[j, d], b2_recv.at[j, y], {"tp": to * CORES + c})
    own_rows = pl.ds(pl.multiple_of(tp * share, share), share)
    for j in range(CHUNKS):
        total = pair_sum(j, y)
        for d in range(1, ny):
            frm = ys(d)
            arrive(r2.at[j, frm], b2_send.at[0, 0], b2_recv.at[j, frm], {"tp": frm * CORES + c})
            total += r2[j, frm].astype(F32)
        per = n_tp // CHUNKS
        mine = jnp.concatenate([xf[t, own_rows, :] for t in range(j * per, (j + 1) * per)], axis=1)
        mid[z, x, j] = (mine.astype(F32) + total).astype(BF16)
        for d in range(1, nz):
            send(mid.at[z, x, j], mid.at[z, x, j], cz_send.at[j, d], c_recv.at[z, x, j], {"kv": zs(d) * nx + x})
        for d in range(1, nx):
            send(mid.at[z, x, j], mid.at[z, x, j], cx_send.at[j, 0, d], c_recv.at[z, x, j], {"kv": z * nx + xs(d)})

    def forward(e):
        for j in range(CHUNKS):
            zz = zs(e)
            arrive(mid.at[zz, x, j], cz_send.at[0, 0], c_recv.at[zz, x, j], {"kv": zz * nx + x})
            for d in range(1, nx):
                send(mid.at[zz, x, j], mid.at[zz, x, j], cx_send.at[j, e, d], c_recv.at[zz, x, j], {"kv": z * nx + xs(d)})

    tall = nx * share
    hidden_units = wu.shape[1]
    up_tile = min(256, hidden_units)
    down_tile = 256

    def mixer(e):
        zz = zs(e)
        for d in range(1, nx):
            for j in range(CHUNKS):
                xx = xs(d)
                arrive(mid.at[zz, xx, j], cz_send.at[0, 0], c_recv.at[zz, xx, j], {"kv": z * nx + xx})
        sums = jnp.zeros((tall, 1), F32)
        for j in range(CHUNKS):
            wide = mid[zz, :, j].reshape(tall, piece).astype(F32)
            sums += jnp.sum(wide * wide, axis=1, keepdims=True)
            lhs[:, j * piece:(j + 1) * piece] = (
                wide * chan_gain[:, j * piece:(j + 1) * piece].astype(F32)
            ).astype(BF16)
        rms = lax.rsqrt(sums * (1.0 / width) + EPSILON)
        if e == 0:
            loads[6 + heads].wait()

        @pl.loop(0, hidden_units // up_tile)
        def _(i):
            at = pl.ds(pl.multiple_of(i * up_tile, up_tile), up_tile)
            hidden = jnp.maximum(dot(lhs[...], wu[:, at]) * rms, 0.0)
            act[:, at] = (hidden * hidden).astype(BF16)

        if e == 0:
            loads[7 + heads].wait()

        @pl.loop(0, width // down_tile)
        def _(i):
            at = pl.ds(pl.multiple_of(i * down_tile, down_tile), down_tile)
            down = dot(act[...], wd[:, at])
            for xx in range(nx):
                sx[e, xx, :, at] = down[xx * share:(xx + 1) * share].astype(BF16)

        for d in range(1, nx):
            xx = xs(d)
            send(sx.at[e, xx], rx.at[e, x], dx_send.at[e, d], dx_recv.at[e, x], {"kv": z * nx + xx})

    def reduce_x(e):
        total = sx[e, x].astype(F32)
        for d in range(1, nx):
            xx = xs(d)
            arrive(rx.at[e, xx], dx_send.at[0, 0], dx_recv.at[e, xx], {"kv": z * nx + xx})
            total += rx[e, xx].astype(F32)
        return total

    def reduce_z(e):
        sz[e] = reduce_x(e).astype(BF16)
        send(sz.at[e], rz.at[z], dz_send.at[e], dz_recv.at[z], {"kv": zs(e) * nx + x})

    for e in range(nz):
        if e + 1 < nz:
            forward(e + 1)
        mixer(e)
        if e >= 2:
            reduce_z(e - 1)
    if nz > 1:
        reduce_z(nz - 1)
    total = reduce_x(0)
    total += jnp.concatenate([mid[z, x, j] for j in range(CHUNKS)], axis=1).astype(F32)
    for d in range(1, nz):
        zz = zs(d)
        arrive(rz.at[zz], dz_send.at[0], dz_recv.at[zz], {"kv": zz * nx + x})
        total += rz[zz].astype(F32)
    done = total.astype(BF16)
    for t in range(n_tp):
        fin[t] = done[:, t * feats:(t + 1) * feats]
    for d in range(1, n_tp):
        to = lax.rem(tp + d, n_tp)
        send(fin.at[to], ob.at[tp], e_send.at[d], e_recv.at[tp], {"tp": to})
    ob[tp] = fin[tp]
    for d in range(1, n_tp):
        frm = lax.rem(tp + d, n_tp)
        arrive(ob.at[frm], e_send.at[0], e_recv.at[frm], {"tp": frm})
    out_ref[...] = ob[...].reshape(rows, feats)
    for copy in sent:
        copy.wait_send()
    for copy in stores:
        copy.wait()


def local(
    n_kv, n_tp,
    tokens, states, mix_gain, w_query, w_key, w_value, w_gate, head_gain, w_output,
    channel_gain, w_up, w_down,
):
    rows, feats = tokens.shape
    heads, head = states.shape[1], states.shape[2]
    width = mix_gain.shape[0]
    inner = w_query.shape[1]
    hidden = w_up.shape[1]
    share = rows // n_tp
    nx = 1
    while (2 * nx) ** 2 <= n_kv:
        nx *= 2
    nz = n_kv // nx
    ny = n_tp // CORES
    piece = width // CHUNKS
    angles = POS * ROTARY_BASE ** (-np.arange(head // 2) / (head // 2))
    turn = np.concatenate([np.cos(angles), np.sin(angles)])[:, None]
    turn = jnp.asarray(np.broadcast_to(turn, (head, rows)), F32)
    sizes = (n_tp, ny, nz, nx, heads, head, rows, feats, share, width)
    hbm = pl.BlockSpec(memory_space=pl.ANY)
    vmem = pl.BlockSpec(memory_space=pltpu.VMEM)
    dma = pltpu.SemaphoreType.DMA
    layer_out, new_states = pl.pallas_call(
        functools.partial(kernel, sizes),
        out_shape=(
            jax.ShapeDtypeStruct((rows, feats), BF16),
            jax.ShapeDtypeStruct((heads, head, head, rows), F32),
        ),
        in_specs=[hbm, hbm, vmem, hbm, hbm, hbm, hbm, vmem, hbm, vmem, hbm, hbm, vmem],
        out_specs=(vmem, hbm),
        scratch_shapes=[
            pltpu.VMEM((n_tp, rows, feats), BF16),
            pltpu.VMEM((4, width, inner), BF16),
            pltpu.VMEM((heads, head, head, rows), F32),
            pltpu.VMEM((inner, width), BF16),
            pltpu.VMEM((width, hidden), BF16),
            pltpu.VMEM((hidden, width), BF16),
            pltpu.VMEM((4, rows, inner), F32),
            pltpu.VMEM((inner, rows), F32),
            pltpu.VMEM((inner, rows), F32),
            pltpu.VMEM((inner, rows), F32),
            pltpu.VMEM((inner, rows), F32),
            pltpu.VMEM((CHUNKS, n_tp, share, piece), BF16),
            pltpu.VMEM((CHUNKS, ny, share, piece), BF16),
            pltpu.VMEM((CHUNKS, ny, share, piece), BF16),
            pltpu.VMEM((CHUNKS, ny, share, piece), BF16),
            pltpu.VMEM((nz, nx, CHUNKS, share, piece), BF16),
            pltpu.VMEM((nx * share, width), BF16),
            pltpu.VMEM((nx * share, hidden), BF16),
            pltpu.VMEM((nz, nx, share, width), BF16),
            pltpu.VMEM((nz, nx, share, width), BF16),
            pltpu.VMEM((nz, share, width), BF16),
            pltpu.VMEM((nz, share, width), BF16),
            pltpu.VMEM((n_tp, share, feats), BF16),
            pltpu.VMEM((n_tp, share, feats), BF16),
            dma((8 + heads,)),
            dma((heads,)),
            dma((2 * ny,)),
            dma((n_tp,)),
            dma((CHUNKS, ny)),
            dma((CHUNKS, ny)),
            dma((CHUNKS, ny)),
            dma((CHUNKS, ny)),
            dma((CHUNKS, nz)),
            dma((CHUNKS, nz, nx)),
            dma((nz, nx, CHUNKS)),
            dma((nz, nx)),
            dma((nz, nx)),
            dma((nz,)),
            dma((nz,)),
            dma((n_tp,)),
            dma((n_tp,)),
        ],
        compiler_params=pltpu.CompilerParams(
            collective_id=0, has_side_effects=True, vmem_limit_bytes=56 * 1024 * 1024
        ),
    )(
        tokens, jnp.transpose(states, (1, 2, 3, 0)), mix_gain[None], w_query, w_key, w_value,
        w_gate, head_gain[None], w_output, channel_gain[None], w_up, w_down, turn,
    )
    return (layer_out, jnp.transpose(new_states, (3, 0, 1, 2)))


def solution(mesh):
    placed = (
        P("kv", "tp"),
        P("kv", "tp", None, None),
        P(),
        P(None, "tp"),
        P(None, "tp"),
        P(None, "tp"),
        P(None, "tp"),
        P("tp"),
        P("tp", None),
        P(),
        P(None, "kv"),
        P("kv", None),
    )
    return jax.shard_map(
        functools.partial(local, mesh.shape["kv"], mesh.shape["tp"]),
        mesh=mesh,
        in_specs=placed,
        out_specs=(P("kv", "tp"), P("kv", "tp", None, None)),
        check_vma=False,
    )
```

```python
import functools
import math

import jax
import jax.numpy as jnp
import numpy as np
from jax import lax
from jax.experimental import pallas as pl
from jax.experimental.pallas import tpu as pltpu
from jax.sharding import PartitionSpec as P

POS = 16384
EPSILON = 1e-06
ROTARY_BASE = 10000.0
CORES = 2
CHUNKS = 2
SLICES = 4
MESH = pl.DeviceIdType.MESH
F32 = jnp.float32
BF16 = jnp.bfloat16


def dot(a, b):
    return jnp.dot(a, b, preferred_element_type=F32)


def kernel(
    sizes,
    tok_hbm, st_hbm, mix_gain, wq_hbm, wk_hbm, wv_hbm, wg_hbm, head_gain, wo_hbm,
    chan_gain, wu_hbm, wd_hbm, turn,
    out_ref, st,
    gain1, gain2, xf, wproj, wo, wu, wd, acc, qt, kt, vt, rt,
    part, r1, s2, r2, mid, lhs, act, sx, rx, sz, rz, fin, ob,
    load_sem, a_send, a_recv, b1_send, b1_recv, b2_send, b2_recv,
    cz_send, cx_send, c_recv, dx_send, dx_recv, dz_send, dz_recv, e_send, e_recv,
):
    n_tp, ny, nz, nx, heads, head, rows, feats, share, width = sizes
    tp = lax.axis_index("tp")
    kv = lax.axis_index("kv")
    c, y = lax.rem(tp, CORES), tp // CORES
    x, z = lax.rem(kv, nx), kv // nx
    other = 1 - c
    partner = y * CORES + other
    half = head // 2
    piece = width // CHUNKS
    strip = width // SLICES
    sent = []

    def ys(d):
        return lax.rem(y + d, ny)

    def zs(d):
        return lax.rem(z + d, nz)

    def xs(d):
        return lax.rem(x + d, nx)

    def make(src, dst, ssem, rsem, device):
        return pltpu.make_async_remote_copy(
            src_ref=src, dst_ref=dst, send_sem=ssem, recv_sem=rsem,
            device_id=device, device_id_type=MESH,
        )

    def send(src, dst, ssem, rsem, device):
        copy = make(src, dst, ssem, rsem, device)
        copy.start()
        sent.append(copy)

    def arrive(dst, ssem, rsem, device):
        make(dst, dst, ssem, rsem, device).wait_recv()

    barrier = pltpu.get_barrier_semaphore()
    greeted = 0
    for d in range(1, n_tp):
        pl.semaphore_signal(barrier, inc=1, device_id={"tp": lax.rem(tp + d, n_tp)}, device_id_type=MESH)
        greeted += 1
    for d in range(1, nx):
        pl.semaphore_signal(barrier, inc=1, device_id={"kv": z * nx + xs(d)}, device_id_type=MESH)
        greeted += 1
    for d in range(1, nz):
        pl.semaphore_signal(barrier, inc=1, device_id={"kv": zs(d) * nx + x}, device_id_type=MESH)
        greeted += 1

    loads = [pltpu.make_async_copy(tok_hbm, xf.at[tp], load_sem.at[0])]
    for i, w in enumerate((wq_hbm, wk_hbm, wv_hbm, wg_hbm)):
        loads.append(pltpu.make_async_copy(w, wproj.at[i], load_sem.at[1 + i]))
    for h in range(heads):
        loads.append(pltpu.make_async_copy(st_hbm.at[h], st.at[h], load_sem.at[5 + h]))
    loads.append(pltpu.make_async_copy(wo_hbm, wo, load_sem.at[5 + heads]))
    loads.append(pltpu.make_async_copy(wu_hbm, wu, load_sem.at[6 + heads]))
    loads.append(pltpu.make_async_copy(wd_hbm, wd, load_sem.at[7 + heads]))
    for copy in loads:
        copy.start()
    gain1[...] = mix_gain[...].astype(F32).reshape(1, width)
    gain2[...] = chan_gain[...].astype(F32).reshape(1, width)
    loads[0].wait()
    pl.semaphore_wait(barrier, greeted)

    for d in range(1, ny):
        send(xf.at[tp], xf.at[tp], a_send.at[d], a_recv.at[tp], {"tp": ys(d) * CORES + c})
    send(xf.at[tp], xf.at[tp], a_send.at[0], a_recv.at[tp], {"tp": partner})

    squares = jnp.zeros((rows, 1), F32)

    def project(slot, first, squares):
        at = pl.ds(pl.multiple_of(slot * feats, feats), feats)
        wide = xf[slot].astype(F32)
        scaled = (wide * gain1[:, at]).astype(BF16)
        for i in range(4):
            if first:
                loads[1 + i].wait()
            term = dot(scaled, wproj[i, at, :])
            if first:
                acc[i] = term
            else:
                acc[i] += term
        return squares + jnp.sum(wide * wide, axis=1, keepdims=True)

    squares = project(tp, True, squares)
    arrive(xf.at[partner], a_send.at[0], a_recv.at[partner], {"tp": partner})
    squares = project(partner, False, squares)
    for d in range(1, ny):
        slot = ys(d) * CORES + c
        arrive(xf.at[slot], a_send.at[0], a_recv.at[slot], {"tp": slot})
        send(xf.at[slot], xf.at[slot], a_send.at[ny + d], a_recv.at[slot], {"tp": partner})
        squares = project(slot, False, squares)
        slot = ys(d) * CORES + other
        arrive(xf.at[slot], a_send.at[0], a_recv.at[slot], {"tp": partner})
        squares = project(slot, False, squares)
    inverse = lax.rsqrt(squares * (1.0 / width) + EPSILON)

    qt[...] = (acc[0] * inverse).T
    kt[...] = (acc[1] * inverse).T
    vt[...] = (acc[2] * inverse).T
    cosine, sine = turn[:half, :], turn[half:, :]
    for h in range(heads):
        lo, hi = pl.ds(h * head, half), pl.ds(h * head + half, half)
        for ref, scale in ((qt, head ** -0.5), (kt, 1.0)):
            a, b = ref[lo, :], ref[hi, :]
            ref[lo, :] = (a * cosine - b * sine) * scale
            ref[hi, :] = (a * sine + b * cosine) * scale
    for h in range(heads):
        loads[5 + h].wait()
        number = (tp * heads + h).astype(F32)
        decay = 1.0 - jnp.exp2(-1.0 - 11.0 * jnp.full((1, rows), number, F32) / (heads * n_tp - 1))
        value = vt[pl.ds(h * head, head), :]
        base = h * head

        def step(k, total, h=h, base=base, decay=decay, value=value):
            fresh = decay * st[h, k] + kt[pl.ds(base + k, 1), :] * value
            st[h, k] = fresh
            return total + qt[pl.ds(base + k, 1), :] * fresh

        total = lax.fori_loop(0, head, step, jnp.zeros((head, rows), F32), unroll=8)
        center = total - jnp.mean(total, axis=0, keepdims=True)
        spread = jnp.mean(center * center, axis=0, keepdims=True)
        rt[pl.ds(base, head), :] = center * lax.rsqrt(spread + EPSILON)
    gating = acc[3] * inverse
    gated = (rt[...].T * head_gain[...].astype(F32).reshape(1, heads * head) * (gating * jax.nn.sigmoid(gating))).astype(BF16)

    loads[5 + heads].wait()
    for j in range(CHUNKS):
        whole = dot(gated, wo[:, j * piece:(j + 1) * piece]).astype(BF16)
        for t in range(n_tp):
            part[j, t] = whole[t * share:(t + 1) * share]
        for d in range(ny):
            to = ys(d)
            send(part.at[j, to * CORES + other], r1.at[j, to], b1_send.at[j, d], b1_recv.at[j, to], {"tp": partner})

    def pair_sum(j, to):
        arrive(r1.at[j, to], b1_send.at[0, 0], b1_recv.at[j, to], {"tp": partner})
        return part[j, to * CORES + c].astype(F32) + r1[j, to].astype(F32)

    for j in range(CHUNKS):
        for d in range(1, ny):
            to = ys(d)
            s2[j, to] = pair_sum(j, to).astype(BF16)
            send(s2.at[j, to], r2.at[j, y], b2_send.at[j, d], b2_recv.at[j, y], {"tp": to * CORES + c})
    own_rows = pl.ds(pl.multiple_of(tp * share, share), share)
    for j in range(CHUNKS):
        total = pair_sum(j, y)
        for d in range(1, ny):
            frm = ys(d)
            arrive(r2.at[j, frm], b2_send.at[0, 0], b2_recv.at[j, frm], {"tp": frm * CORES + c})
            total += r2[j, frm].astype(F32)
        per = n_tp // CHUNKS
        mine = jnp.concatenate([xf[t, own_rows, :] for t in range(j * per, (j + 1) * per)], axis=1)
        mid[z, x, j] = (mine.astype(F32) + total).astype(BF16)
        for d in range(1, nz):
            send(mid.at[z, x, j], mid.at[z, x, j], cz_send.at[j, d], c_recv.at[z, x, j], {"kv": zs(d) * nx + x})
        for d in range(1, nx):
            send(mid.at[z, x, j], mid.at[z, x, j], cx_send.at[j, 0, d], c_recv.at[z, x, j], {"kv": z * nx + xs(d)})

    def forward(e):
        for j in range(CHUNKS):
            zz = zs(e)
            arrive(mid.at[zz, x, j], cz_send.at[0, 0], c_recv.at[zz, x, j], {"kv": zz * nx + x})
            for d in range(1, nx):
                send(mid.at[zz, x, j], mid.at[zz, x, j], cx_send.at[j, e, d], c_recv.at[zz, x, j], {"kv": z * nx + xs(d)})

    tall = nx * share
    hidden_units = wu.shape[1]
    up_tile = min(256, hidden_units)
    down_tile = 256

    def mixer(e):
        zz = zs(e)
        for d in range(1, nx):
            for j in range(CHUNKS):
                xx = xs(d)
                arrive(mid.at[zz, xx, j], cz_send.at[0, 0], c_recv.at[zz, xx, j], {"kv": z * nx + xx})
        sums = jnp.zeros((tall, 1), F32)
        for j in range(CHUNKS):
            wide = mid[zz, :, j].reshape(tall, piece).astype(F32)
            sums += jnp.sum(wide * wide, axis=1, keepdims=True)
            lhs[:, j * piece:(j + 1) * piece] = (
                wide * gain2[:, j * piece:(j + 1) * piece]
            ).astype(BF16)
        rms = lax.rsqrt(sums * (1.0 / width) + EPSILON)
        if e == 0:
            loads[6 + heads].wait()

        @pl.loop(0, hidden_units // up_tile)
        def _(i):
            at = pl.ds(pl.multiple_of(i * up_tile, up_tile), up_tile)
            hidden = jnp.maximum(dot(lhs[...], wu[:, at]) * rms, 0.0)
            act[:, at] = (hidden * hidden).astype(BF16)

        if e == 0:
            loads[7 + heads].wait()

        for q in range(SLICES):
            for i in range(strip // down_tile):
                down = dot(act[...], wd[:, q * strip + i * down_tile:q * strip + (i + 1) * down_tile])
                for xx in range(nx):
                    sx[e, xx, q, :, i * down_tile:(i + 1) * down_tile] = (
                        down[xx * share:(xx + 1) * share].astype(BF16)
                    )
            for d in range(1, nx):
                xx = xs(d)
                send(sx.at[e, xx, q], rx.at[e, x, q], dx_send.at[e, d, q], dx_recv.at[e, x, q], {"kv": z * nx + xx})

    def reduce_x(e, q):
        total = sx[e, x, q].astype(F32)
        for d in range(1, nx):
            xx = xs(d)
            arrive(rx.at[e, xx, q], dx_send.at[0, 0, 0], dx_recv.at[e, xx, q], {"kv": z * nx + xx})
            total += rx[e, xx, q].astype(F32)
        return total

    def reduce_z(e):
        for q in range(SLICES):
            sz[e, q] = reduce_x(e, q).astype(BF16)
            send(sz.at[e, q], rz.at[z, q], dz_send.at[e, q], dz_recv.at[z, q], {"kv": zs(e) * nx + x})

    for e in range(nz):
        if e + 1 < nz:
            forward(e + 1)
        mixer(e)
        if e >= 2:
            reduce_z(e - 1)
    if nz > 1:
        reduce_z(nz - 1)
    per_piece, per_strip = piece // strip, strip // feats
    for q in range(SLICES):
        inside = q % per_piece
        total = reduce_x(0, q)
        total += mid[z, x, q // per_piece, :, inside * strip:(inside + 1) * strip].astype(F32)
        for d in range(1, nz):
            zz = zs(d)
            arrive(rz.at[zz, q], dz_send.at[0, 0], dz_recv.at[zz, q], {"kv": zz * nx + x})
            total += rz[zz, q].astype(F32)
        done = total.astype(BF16)
        for i in range(per_strip):
            t = q * per_strip + i
            fin[t] = done[:, i * feats:(i + 1) * feats]

            @pl.when(tp != t)
            def _(t=t):
                make(fin.at[t], ob.at[tp], e_send.at[t], e_recv.at[tp], {"tp": t}).start()

            @pl.when(tp == t)
            def _(t=t):
                ob[tp] = fin[t]

    for d in range(1, n_tp):
        frm = lax.rem(tp + d, n_tp)
        arrive(ob.at[frm], e_send.at[0], e_recv.at[frm], {"tp": frm})
        make(fin.at[frm], ob.at[tp], e_send.at[frm], e_recv.at[tp], {"tp": frm}).wait_send()
    out_ref[...] = ob[...].reshape(rows, feats)
    for copy in sent:
        copy.wait_send()


def local(
    n_kv, n_tp,
    tokens, states, mix_gain, w_query, w_key, w_value, w_gate, head_gain, w_output,
    channel_gain, w_up, w_down,
):
    rows, feats = tokens.shape
    heads, head = states.shape[1], states.shape[2]
    width = mix_gain.shape[0]
    inner = w_query.shape[1]
    hidden = w_up.shape[1]
    share = rows // n_tp
    nx = 1
    while (2 * nx) ** 2 <= n_kv:
        nx *= 2
    nz = n_kv // nx
    ny = n_tp // CORES
    piece = width // CHUNKS
    strip = width // SLICES
    angles = POS * ROTARY_BASE ** (-np.arange(head // 2) / (head // 2))
    turn = np.concatenate([np.cos(angles), np.sin(angles)])[:, None]
    turn = jnp.asarray(np.broadcast_to(turn, (head, rows)), F32)
    sizes = (n_tp, ny, nz, nx, heads, head, rows, feats, share, width)
    hbm = pl.BlockSpec(memory_space=pltpu.HBM)
    vmem = pl.BlockSpec(memory_space=pltpu.VMEM)
    dma = pltpu.SemaphoreType.DMA
    layer_out, new_states = pl.pallas_call(
        functools.partial(kernel, sizes),
        out_shape=(
            pltpu.VMEM((rows, feats), BF16),
            pltpu.VMEM((heads, head, head, rows), F32),
        ),
        in_specs=[hbm, hbm, vmem, hbm, hbm, hbm, hbm, vmem, hbm, vmem, hbm, hbm, vmem],
        out_specs=(vmem, vmem),
        scratch_shapes=[
            pltpu.VMEM((1, width), F32),
            pltpu.VMEM((1, width), F32),
            pltpu.VMEM((n_tp, rows, feats), BF16),
            pltpu.VMEM((4, width, inner), BF16),
            pltpu.VMEM((inner, width), BF16),
            pltpu.VMEM((width, hidden), BF16),
            pltpu.VMEM((hidden, width), BF16),
            pltpu.VMEM((4, rows, inner), F32),
            pltpu.VMEM((inner, rows), F32),
            pltpu.VMEM((inner, rows), F32),
            pltpu.VMEM((inner, rows), F32),
            pltpu.VMEM((inner, rows), F32),
            pltpu.VMEM((CHUNKS, n_tp, share, piece), BF16),
            pltpu.VMEM((CHUNKS, ny, share, piece), BF16),
            pltpu.VMEM((CHUNKS, ny, share, piece), BF16),
            pltpu.VMEM((CHUNKS, ny, share, piece), BF16),
            pltpu.VMEM((nz, nx, CHUNKS, share, piece), BF16),
            pltpu.VMEM((nx * share, width), BF16),
            pltpu.VMEM((nx * share, hidden), BF16),
            pltpu.VMEM((nz, nx, SLICES, share, strip), BF16),
            pltpu.VMEM((nz, nx, SLICES, share, strip), BF16),
            pltpu.VMEM((nz, SLICES, share, strip), BF16),
            pltpu.VMEM((nz, SLICES, share, strip), BF16),
            pltpu.VMEM((n_tp, share, feats), BF16),
            pltpu.VMEM((n_tp, share, feats), BF16),
            dma((8 + heads,)),
            dma((2 * ny,)),
            dma((n_tp,)),
            dma((CHUNKS, ny)),
            dma((CHUNKS, ny)),
            dma((CHUNKS, ny)),
            dma((CHUNKS, ny)),
            dma((CHUNKS, nz)),
            dma((CHUNKS, nz, nx)),
            dma((nz, nx, CHUNKS)),
            dma((nz, nx, SLICES)),
            dma((nz, nx, SLICES)),
            dma((nz, SLICES)),
            dma((nz, SLICES)),
            dma((n_tp,)),
            dma((n_tp,)),
        ],
        compiler_params=pltpu.CompilerParams(
            collective_id=0, has_side_effects=True, vmem_limit_bytes=48 * 1024 * 1024
        ),
    )(
        tokens, jnp.transpose(states, (1, 2, 3, 0)), mix_gain, w_query, w_key, w_value,
        w_gate, head_gain, w_output, channel_gain, w_up, w_down, turn,
    )
    return (layer_out, jnp.transpose(new_states, (3, 0, 1, 2)))


def solution(mesh):
    placed = (
        P("kv", "tp"),
        P("kv", "tp", None, None),
        P(),
        P(None, "tp"),
        P(None, "tp"),
        P(None, "tp"),
        P(None, "tp"),
        P("tp"),
        P("tp", None),
        P(),
        P(None, "kv"),
        P("kv", None),
    )
    return jax.shard_map(
        functools.partial(local, mesh.shape["kv"], mesh.shape["tp"]),
        mesh=mesh,
        in_specs=placed,
        out_specs=(P("kv", "tp"), P("kv", "tp", None, None)),
        check_vma=False,
    )
```
